32 devices in a mesh: kv: 8 (over z, y), tp: 4 (over x, core).
Axes of the slice: x: 2, y: 2, z: 4, core: 2. Of those that a mesh axis runs over, the one named last changes fastest.
Arguments:
- hidden_rows: bfloat16 [128, 4096], P('kv', 'tp'), may hold values from -16 to 16
- carried_state: float32 [128, 524288], P('kv', 'tp'), may hold values from -6 to 6
- norm_gain: bfloat16 [4096], replicated, may hold values from 0.099609375 to 1.8984375
- w_query: bfloat16 [4096, 2048], P('kv', 'tp'), may hold values from -0.09375 to 0.09375
- w_key: bfloat16 [4096, 2048], P('kv', 'tp'), may hold values from -0.09375 to 0.09375
- w_decay: bfloat16 [4096, 2048], P('kv', 'tp'), may hold values from -0.375 to 0.375
- w_value: bfloat16 [4096, 4096], P('kv', 'tp'), may hold values from -0.09375 to 0.09375
- w_gate: bfloat16 [4096, 4096], P('kv', 'tp'), may hold values from -0.09375 to 0.09375
- decay_bias: float32 [2048], P('tp'), may hold values from -32 to 8
- head_gain: bfloat16 [256], replicated, may hold values from 0.099609375 to 1.8984375
- w_out: bfloat16 [4096, 4096], P('tp', 'kv'), may hold values from -0.09375 to 0.09375
- mlp_gain: bfloat16 [4096], P('tp'), may hold values from 0.099609375 to 1.8984375
- w_up: bfloat16 [4096, 16384], P('tp', 'kv'), may hold values from -0.09375 to 0.09375
- w_down: bfloat16 [16384, 4096], P('kv', 'tp'), may hold values from -0.046875 to 0.046875
Outputs:
- updated_rows: bfloat16 [128, 4096], P('kv', 'tp')
- new_state: float32 [128, 524288], P('kv', 'tp')
The draws below stay inside these ranges and needn't reach their ends.
All inputs are finite; a program needn't handle non-finite values.
Results may differ from the reference program's by a relative error of at most 0.025.
Values may be sent and summed in bfloat16 or wider, within the bound.
A program may use at most 128 MiB of HBM per device.

```python
import jax
import jax.numpy as jnp
from jax import lax

D = 4096
HEADS = 16
DK = 128
DV = 256
FF = 16384
BATCH = 128
N_TP = 4


def draw_hidden_rows(key, part):
    key_base = jax.random.fold_in(key, 11)
    key_rough = jax.random.fold_in(key, 12)
    columns = jnp.arange(D, dtype=jnp.float32)
    rising = 0.5 * jnp.power(4.0, columns / D)
    rough = jnp.exp(jax.random.uniform(key_rough, (D,), jnp.float32, -0.35, 0.35))
    base = jnp.clip(jax.random.normal(key_base, (BATCH, D), jnp.float32), -5.0, 5.0)
    return (base * rising[None, :] * rough[None, :]).astype(jnp.bfloat16)


def shard_levels(rng, shape, pieces, smallest, largest):
    factor_of, own = 1.0, jax.random.fold_in(rng, 6)
    for dim, blocks in pieces:
        draws = jnp.exp(jax.random.uniform(jax.random.fold_in(own, dim), (blocks,), jnp.float32, smallest / len(pieces), largest / len(pieces)))
        factor_of = factor_of * jnp.repeat(draws, shape[dim] // blocks).reshape([-1 if axis == dim else 1 for axis in range(len(shape))])
    return factor_of


def normal_values(key, shape, deviation, bound, split=(), kind=jnp.bfloat16):
    entries = jax.random.normal(key, shape, jnp.float32) * deviation
    if len(split) > 0:
        entries = shard_levels(key, shape, split, -0.22, 0.18) * entries
    return jnp.clip(entries, min=-bound, max=bound).astype(kind)


def setup_inputs(seed: int = 0) -> dict:
    keys = jax.random.split(jax.random.key(seed), 15)
    hidden_rows = draw_hidden_rows(jax.random.fold_in(keys[14], 71), 0)
    carried_state = normal_values(keys[1], (BATCH, HEADS * DK * DV), 1.0, 6.0, ((0, 8), (1, 4)), jnp.float32)
    norm_gain = jnp.clip(1.0 + 0.18 * jax.random.normal(keys[2], (D,), jnp.float32), 0.099609375, 1.8984375).astype(jnp.bfloat16)
    w_query = normal_values(keys[3], (D, HEADS * DK), D ** -0.5, 0.09375, ((0, 8), (1, 4)))
    w_key = normal_values(keys[4], (D, HEADS * DK), D ** -0.5, 0.09375, ((0, 8), (1, 4)))
    w_decay = normal_values(keys[5], (D, HEADS * DK), (D // 16) ** -0.5, 0.375, ((0, 8), (1, 4)))
    w_value = normal_values(keys[6], (D, HEADS * DV), D ** -0.5, 0.09375, ((0, 8), (1, 4)))
    w_gate = normal_values(keys[7], (D, HEADS * DV), D ** -0.5, 0.09375, ((0, 8), (1, 4)))
    decay_bias = jnp.clip(-32.0 + 40.0 * jax.random.uniform(keys[8], (HEADS * DK,), jnp.float32) ** shard_levels(keys[8], (HEADS * DK,), ((0, 4),), -0.2, 0.2), -32.0, 8.0)
    head_gain = jnp.clip(1.0 + 0.18 * jax.random.normal(keys[9], (DV,), jnp.float32), 0.099609375, 1.8984375).astype(jnp.bfloat16)
    w_out = normal_values(keys[10], (HEADS * DV, D), (HEADS * DV) ** -0.5, 0.09375, ((0, 4), (1, 8)))
    mlp_gain = jnp.clip(1.0 + 0.18 * jax.random.normal(keys[11], (D,), jnp.float32), 0.099609375, 1.8984375).astype(jnp.bfloat16)
    w_up = normal_values(keys[12], (D, FF), D ** -0.5, 0.09375, ((0, 4), (1, 8)))
    w_down = normal_values(keys[13], (FF, D), FF ** -0.5, 0.046875, ((0, 8), (1, 4)))
    return dict(hidden_rows=hidden_rows, carried_state=carried_state, norm_gain=norm_gain, w_query=w_query, w_key=w_key, w_decay=w_decay, w_value=w_value, w_gate=w_gate, decay_bias=decay_bias, head_gain=head_gain, w_out=w_out, mlp_gain=mlp_gain, w_up=w_up, w_down=w_down)


epsilon = 1e-06
decay_normalizer = 16.0

def reference(hidden_rows, carried_state, norm_gain, w_query, w_key, w_decay, w_value, w_gate, decay_bias, head_gain, w_out, mlp_gain, w_up, w_down):
    batch_rows = hidden_rows.shape[0]
    inputs = hidden_rows.astype(jnp.float32)
    normed = (inputs * lax.rsqrt(lax.optimization_barrier(jnp.mean(inputs * inputs, axis=-1, keepdims=True)) + epsilon) * norm_gain.astype(jnp.float32)).astype(jnp.bfloat16)
    queries = jnp.dot(normed, w_query, preferred_element_type=jnp.float32).astype(jnp.bfloat16)
    keys_new = jnp.dot(normed, w_key, preferred_element_type=jnp.float32).astype(jnp.bfloat16)
    decay_pre = jnp.dot(normed, w_decay, preferred_element_type=jnp.float32).astype(jnp.bfloat16)
    values = jnp.dot(normed, w_value, preferred_element_type=jnp.float32).astype(jnp.bfloat16)
    out_gate = jnp.dot(normed, w_gate, preferred_element_type=jnp.float32).astype(jnp.bfloat16)
    log_decay = jax.nn.log_sigmoid(decay_pre.astype(jnp.float32) + decay_bias) / decay_normalizer
    log_decay = log_decay.reshape(batch_rows, HEADS, DK)
    carried = carried_state.reshape(batch_rows, HEADS, DK, DV)
    key_heads = keys_new.astype(jnp.float32).reshape(batch_rows, HEADS, DK)
    value_heads = values.astype(jnp.float32).reshape(batch_rows, HEADS, DV)
    new_state = jnp.exp(log_decay)[..., None] * carried + key_heads[..., None] * value_heads[..., None, :]
    query_heads = queries.astype(jnp.float32).reshape(batch_rows, HEADS, DK) * DK ** (-0.5)
    head_out = jnp.einsum('bhk,bhkv->bhv', query_heads, new_state, precision=lax.Precision.HIGHEST)
    gate_heads = out_gate.astype(jnp.float32).reshape(batch_rows, HEADS, DV)
    mixed = head_out * lax.rsqrt(lax.optimization_barrier(jnp.mean(head_out * head_out, axis=-1, keepdims=True)) + epsilon)
    mixed = (mixed * head_gain.astype(jnp.float32) * jax.nn.silu(gate_heads)).astype(jnp.bfloat16)
    mixed = mixed.reshape(batch_rows, HEADS * DV)
    group_rows = HEADS * DV // N_TP
    attn_total = jnp.zeros((batch_rows, D), jnp.float32)
    for block in range(N_TP):
        low = block * group_rows
        piece = jnp.dot(mixed[:, low:low + group_rows], w_out[low:low + group_rows], preferred_element_type=jnp.float32).astype(jnp.bfloat16)
        piece = lax.optimization_barrier(piece)
        attn_total = attn_total + piece.astype(jnp.float32)
    attn_out = attn_total.astype(jnp.bfloat16)
    residual = (inputs + attn_out.astype(jnp.float32)).astype(jnp.bfloat16)
    resid_float = residual.astype(jnp.float32)
    row_scale = lax.rsqrt(lax.optimization_barrier(jnp.mean(resid_float * resid_float, axis=-1, keepdims=True)) + epsilon)
    mlp_input = (resid_float * row_scale * mlp_gain.astype(jnp.float32)).astype(jnp.bfloat16)
    feature_block = D // N_TP
    up_sum = jnp.zeros((batch_rows, FF), jnp.float32)
    for block in range(N_TP):
        low = block * feature_block
        piece = jnp.dot(mlp_input[:, low:low + feature_block], w_up[low:low + feature_block], preferred_element_type=jnp.float32).astype(jnp.bfloat16)
        piece = lax.optimization_barrier(piece)
        up_sum = up_sum + piece.astype(jnp.float32)
    activation = jnp.square(jax.nn.relu(up_sum)).astype(jnp.bfloat16)
    mlp_out = jnp.dot(activation, w_down, preferred_element_type=jnp.float32).astype(jnp.bfloat16)
    updated_rows = (resid_float + mlp_out.astype(jnp.float32)).astype(jnp.bfloat16)
    return (updated_rows, new_state.reshape(batch_rows, HEADS * DK * DV))
```

```python
import functools

import jax
import jax.numpy as jnp
from jax import lax
from jax.experimental import pallas as pl
from jax.experimental.pallas import tpu as pltpu
from jax.sharding import PartitionSpec as P

DK = 128
DV = 256

epsilon = 1e-06
decay_normalizer = 16.0

F32 = jnp.float32
BF16 = jnp.bfloat16
MESH = pl.DeviceIdType.MESH


def remote(src, dst, send_sem, recv_sem, i, j):
    return pltpu.make_async_remote_copy(
        src_ref=src,
        dst_ref=dst,
        send_sem=send_sem,
        recv_sem=recv_sem,
        device_id={"kv": i, "tp": j},
        device_id_type=MESH,
    )


def dot(a, b):
    return jnp.dot(a, b, preferred_element_type=F32)


def project_kernel(
    kv, tp, h_ref, g_ref, w0, w1, w2, w3, w4, o0, o1, o2, o3, o4,
    xbuf, v0, v1, v2, v3, v4, s0, s1, s2, s3, s4, r0, r1, r2, r3, r4,
    ssq, wsem, xs_sem, xr_sem, ss_sem, sr_sem, ps_sem, pr_sem,
):
    i, j = lax.axis_index("kv"), lax.axis_index("tp")
    ratio = kv // tp
    rows = h_ref.shape[0]
    width = xbuf.shape[2]
    owner = i // ratio
    ws, vs, outs = (w0, w1, w2, w3, w4), (v0, v1, v2, v3, v4), (o0, o1, o2, o3, o4)
    sends, recvs = (s0, s1, s2, s3, s4), (r0, r1, r2, r3, r4)
    loads = [pltpu.make_async_copy(w, v, wsem.at[n]) for n, (w, v) in enumerate(zip(ws, vs))]

    hidden_sends = []
    for a in range(ratio):
        for s in range(tp):
            dst_i, dst_j = j * ratio + a, lax.rem(j + s, tp)
            src = h_ref.at[:, pl.ds(a * width, width)]
            copy = remote(
                src, xbuf.at[i], xs_sem.at[a * tp + s], xr_sem.at[i], dst_i, dst_j
            )
            hidden_sends.append((a, s, dst_i, copy))
    for a, s, dst_i, copy in hidden_sends:
        if s:
            copy.start()
        else:
            pl.when(dst_i != i)(copy.start)
    for load in loads:
        load.start()

    hidden = h_ref[...].astype(F32)
    ssq[j] = jnp.broadcast_to(jnp.sum(hidden * hidden, axis=1, keepdims=True), (rows, 128))
    for a, s, dst_i, copy in hidden_sends:
        if not s:

            @pl.when(dst_i == i)
            def _():
                xbuf[i] = h_ref[:, a * width : (a + 1) * width]

    for s in range(kv):
        k = lax.rem(i + s, kv)
        arrive = remote(xbuf.at[k], xbuf.at[k], xs_sem.at[0], xr_sem.at[k], k, owner)
        if s:
            arrive.wait_recv()
        else:
            pl.when(owner != j)(arrive.wait_recv)

    square_sends = [
        remote(ssq.at[j], ssq.at[j], ss_sem.at[s], sr_sem.at[j], i, lax.rem(j + s, tp))
        for s in range(1, tp)
    ]
    gain = g_ref[:, pl.ds(pl.multiple_of(i * width, 128), width)].astype(F32)
    x = (xbuf[...].reshape(kv * rows, width).astype(F32) * gain).astype(BF16)
    part_sends = []
    for n in range(5):
        loads[n].wait()
        part = dot(x, vs[n][...]).astype(BF16)
        sends[n][...] = part.reshape(sends[n].shape)
        for s in range(1, kv):
            k = lax.rem(i + s, kv)
            copy = remote(
                sends[n].at[k], recvs[n].at[i], ps_sem.at[n, s], pr_sem.at[n, i], k, j
            )
            copy.start()
            part_sends.append(copy)
        if n == 0:
            for copy in square_sends:
                copy.start()
    for s in range(1, tp):
        k = lax.rem(j + s, tp)
        remote(ssq.at[k], ssq.at[k], ss_sem.at[0], sr_sem.at[k], i, k).wait_recv()
    total = ssq[0]
    for s in range(1, tp):
        total = total + ssq[s]
    scale = lax.rsqrt(total[:, :1] / (kv * width) + epsilon)
    for n in range(5):
        acc = sends[n][i].astype(F32)
        for s in range(1, kv):
            k = lax.rem(i + s, kv)
            remote(
                recvs[n].at[k], recvs[n].at[k], ps_sem.at[n, 0], pr_sem.at[n, k], k, j
            ).wait_recv()
            acc = acc + recvs[n][k].astype(F32)
        outs[n][...] = (acc * scale).astype(BF16)
    for a, s, dst_i, copy in hidden_sends:
        if s:
            copy.wait_send()
        else:
            pl.when(dst_i != i)(copy.wait_send)
    for copy in square_sends + part_sends:
        copy.wait_send()


def project(kv, tp, hidden_rows, norm_gain, weights):
    rows = hidden_rows.shape[0]
    width = weights[0].shape[0]
    vmem = pl.BlockSpec(memory_space=pltpu.VMEM)
    anywhere = pl.BlockSpec(memory_space=pl.ANY)
    slots = [pltpu.VMEM((kv, rows, w.shape[1]), BF16) for w in weights]
    dma = pltpu.SemaphoreType.DMA
    return pl.pallas_call(
        functools.partial(project_kernel, kv, tp),
        out_shape=[jax.ShapeDtypeStruct((rows, w.shape[1]), BF16) for w in weights],
        in_specs=[vmem] * 2 + [anywhere] * 5,
        out_specs=[vmem] * 5,
        scratch_shapes=[pltpu.VMEM((kv, rows, width), BF16)]
        + [pltpu.VMEM(w.shape, BF16) for w in weights]
        + slots
        + slots
        + [
            pltpu.VMEM((tp, rows, 128), F32),
            dma((5,)),
            dma((kv,)),
            dma((kv,)),
            dma((tp,)),
            dma((tp,)),
            dma((5, kv)),
            dma((5, kv)),
        ],
        compiler_params=pltpu.CompilerParams(
            has_side_effects=True, vmem_limit_bytes=32 * 1024 * 1024
        ),
        name="project",
    )(hidden_rows, norm_gain.reshape(1, -1), *weights)


def tail_kernel(
    kv, tp, mixed_ref, h_ref, g_ref, wo, wu, wd, out_ref,
    vo, vu, vd, mall, psend, precv, resid, rall, ssq, usend, urecv, xsend, xrecv, act, dsend, drecv,
    wsem, ms_sem, mr_sem, ps_sem, pr_sem, rs_sem, rr_sem, ss_sem, sr_sem,
    us_sem, ur_sem, xs_sem, xr_sem, as_sem, ar_sem, ds_sem, dr_sem,
):
    i, j = lax.axis_index("kv"), lax.axis_index("tp")
    ratio = kv // tp
    rows, columns = h_ref.shape
    width = columns // ratio
    owner = i // ratio
    loads = [
        pltpu.make_async_copy(w, v, wsem.at[n])
        for n, (w, v) in enumerate(((wo, vo), (wu, vu), (wd, vd)))
    ]
    sent = []

    def everyone(src_of, dst, send_sem, recv_sem):
        for s in range(1, kv):
            k = lax.rem(i + s, kv)
            copy = remote(src_of(k), dst.at[i], send_sem.at[s], recv_sem.at[i], k, j)
            copy.start()
            sent.append(copy)

    def arrived(dst, send_sem, recv_sem, s):
        k = lax.rem(i + s, kv)
        remote(dst.at[k], dst.at[k], send_sem.at[0], recv_sem.at[k], k, j).wait_recv()
        return k

    everyone(lambda k: mixed_ref, mall, ms_sem, mr_sem)
    for load in loads:
        load.start()
    mall[i] = mixed_ref[...]
    for s in range(1, kv):
        arrived(mall, ms_sem, mr_sem, s)
    loads[0].wait()
    part = dot(mall[...].reshape(kv * rows, mall.shape[2]), vo[...]).astype(BF16)
    psend[...] = part.reshape(psend.shape)

    slot = j * ratio + lax.rem(i, ratio)
    own_send = remote(psend.at[i], precv.at[slot], ps_sem.at[0], pr_sem.at[slot], i, owner)
    for s in range(1, kv):
        k = lax.rem(i + s, kv)
        copy = remote(psend.at[k], precv.at[slot], ps_sem.at[s], pr_sem.at[slot], k, owner)
        copy.start()
        sent.append(copy)
    pl.when(owner != j)(own_send.start)

    @pl.when(owner == j)
    def _():
        precv[slot] = psend[i]

    pieces = []
    for a in range(ratio):
        src_i = j * ratio + a
        attn = None
        for s in range(tp):
            src_j = lax.rem(j + s, tp)
            at = src_j * ratio + a
            arrive = remote(precv.at[at], precv.at[at], ps_sem.at[0], pr_sem.at[at], src_i, src_j)
            if s:
                arrive.wait_recv()
            else:
                pl.when(src_i != i)(arrive.wait_recv)
            term = precv[at].astype(F32)
            attn = term if attn is None else attn + term
        hidden = h_ref[:, a * width : (a + 1) * width].astype(F32)
        piece = (hidden + attn.astype(BF16).astype(F32)).astype(BF16)
        resid[:, a * width : (a + 1) * width] = piece
        piece = piece.astype(F32)
        pieces.append(jnp.sum(piece * piece, axis=1, keepdims=True))

    everyone(lambda k: resid, rall, rs_sem, rr_sem)
    ssq[j] = jnp.broadcast_to(sum(pieces), (rows, 128))
    rall[i] = resid[...]
    loads[1].wait()
    for s in range(1, kv):
        arrived(rall, rs_sem, rr_sem, s)
    for s in range(1, tp):
        copy = remote(ssq.at[j], ssq.at[j], ss_sem.at[s], sr_sem.at[j], i, lax.rem(j + s, tp))
        copy.start()
        sent.append(copy)
    x = (rall[...].reshape(kv * rows, columns).astype(F32) * g_ref[...].astype(F32)).astype(BF16)

    half = vu.shape[1] // 2
    core, across = lax.rem(j, 2), j // 2
    other = 1 - core
    partner = across * 2 + other
    usend[...] = dot(x, vu[:, pl.ds(pl.multiple_of(other * half, 128), half)]).astype(BF16)
    give = remote(usend, urecv, us_sem, ur_sem, i, partner)
    give.start()
    mine = dot(x, vu[:, pl.ds(pl.multiple_of(core * half, 128), half)])
    give.wait_recv()
    mine = (mine + urecv[...].astype(F32)).astype(BF16)
    xsend[...] = mine
    for s in range(1, tp // 2):
        to = lax.rem(across + s, tp // 2)
        copy = remote(
            xsend, xrecv.at[across], xs_sem.at[s], xr_sem.at[across], i, to * 2 + core
        )
        copy.start()
        sent.append(copy)
    loads[2].wait()
    total = xsend[...].astype(F32)
    for s in range(1, tp // 2):
        at = lax.rem(across + s, tp // 2)
        remote(
            xrecv.at[at], xrecv.at[at], xs_sem.at[0], xr_sem.at[at], i, at * 2 + core
        ).wait_recv()
        total = total + xrecv[at].astype(F32)
    act[core] = jnp.square(jnp.maximum(total, 0.0)).astype(BF16)
    share = remote(act.at[core], act.at[core], as_sem, ar_sem.at[core], i, partner)
    share.start()
    down = dot(act[core], vd[pl.ds(pl.multiple_of(core * half, 128), half), :])
    remote(act.at[other], act.at[other], as_sem, ar_sem.at[other], i, partner).wait_recv()
    down = down + dot(act[other], vd[pl.ds(pl.multiple_of(other * half, 128), half), :])
    dsend[...] = down.astype(BF16).reshape(dsend.shape)
    everyone(lambda k: dsend.at[k], drecv, ds_sem, dr_sem)

    for s in range(1, tp):
        k = lax.rem(j + s, tp)
        remote(ssq.at[k], ssq.at[k], ss_sem.at[0], sr_sem.at[k], i, k).wait_recv()
    squares = ssq[0]
    for s in range(1, tp):
        squares = squares + ssq[s]
    scale = lax.rsqrt(squares[:, :1] / (columns * tp) + epsilon)
    acc = dsend[i].astype(F32)
    for s in range(1, kv):
        k = arrived(drecv, ds_sem, dr_sem, s)
        acc = acc + drecv[k].astype(F32)
    acc = (acc * (scale * scale)).astype(BF16)
    out_ref[...] = (resid[...].astype(F32) + acc.astype(F32)).astype(BF16)
    give.wait_send()
    share.wait_send()
    pl.when(owner != j)(own_send.wait_send)
    for copy in sent:
        copy.wait_send()


def tail(kv, tp, mixed, hidden_rows, mlp_gain, w_out, w_up, w_down):
    rows, columns = hidden_rows.shape
    width = w_out.shape[1]
    ratio = kv // tp
    half = w_up.shape[1] // 2
    everything = kv * rows
    vmem = pl.BlockSpec(memory_space=pltpu.VMEM)
    anywhere = pl.BlockSpec(memory_space=pl.ANY)
    dma = pltpu.SemaphoreType.DMA
    return pl.pallas_call(
        functools.partial(tail_kernel, kv, tp),
        out_shape=jax.ShapeDtypeStruct((rows, columns), BF16),
        in_specs=[vmem] * 3 + [anywhere] * 3,
        out_specs=vmem,
        scratch_shapes=[
            pltpu.VMEM(w_out.shape, BF16),
            pltpu.VMEM(w_up.shape, BF16),
            pltpu.VMEM(w_down.shape, BF16),
            pltpu.VMEM((kv, rows, mixed.shape[1]), BF16),
            pltpu.VMEM((kv, rows, width), BF16),
            pltpu.VMEM((tp * ratio, rows, width), BF16),
            pltpu.VMEM((rows, columns), BF16),
            pltpu.VMEM((kv, rows, columns), BF16),
            pltpu.VMEM((tp, rows, 128), F32),
            pltpu.VMEM((everything, half), BF16),
            pltpu.VMEM((everything, half), BF16),
            pltpu.VMEM((everything, half), BF16),
            pltpu.VMEM((tp // 2, everything, half), BF16),
            pltpu.VMEM((2, everything, half), BF16),
            pltpu.VMEM((kv, rows, columns), BF16),
            pltpu.VMEM((kv, rows, columns), BF16),
            dma((3,)),
            dma((kv,)),
            dma((kv,)),
            dma((kv,)),
            dma((tp * ratio,)),
            dma((kv,)),
            dma((kv,)),
            dma((tp,)),
            dma((tp,)),
            dma(()),
            dma(()),
            dma((tp // 2,)),
            dma((tp // 2,)),
            dma(()),
            dma((2,)),
            dma((kv,)),
            dma((kv,)),
        ],
        compiler_params=pltpu.CompilerParams(
            has_side_effects=True, vmem_limit_bytes=32 * 1024 * 1024
        ),
        name="tail",
    )(mixed, hidden_rows, mlp_gain.reshape(1, -1), w_out, w_up, w_down)


def body(
    kv,
    tp,
    hidden_rows,
    carried_state,
    norm_gain,
    w_query,
    w_key,
    w_decay,
    w_value,
    w_gate,
    decay_bias,
    head_gain,
    w_out,
    mlp_gain,
    w_up,
    w_down,
):
    seq_rows = hidden_rows.shape[0]
    heads_here = decay_bias.shape[0] // DK
    queries, keys_new, decay_pre, values, out_gate = project(
        kv, tp, hidden_rows, norm_gain, (w_query, w_key, w_decay, w_value, w_gate)
    )
    log_decay = jax.nn.log_sigmoid(decay_pre.astype(F32) + decay_bias) / decay_normalizer
    log_decay = log_decay.reshape(seq_rows, heads_here, DK)
    carried = carried_state.reshape(seq_rows, heads_here, DK, DV)
    key_heads = keys_new.astype(F32).reshape(seq_rows, heads_here, DK)
    value_heads = values.astype(F32).reshape(seq_rows, heads_here, DV)
    new_state = (
        jnp.exp(log_decay)[..., None] * carried + key_heads[..., None] * value_heads[..., None, :]
    )
    query_heads = queries.astype(F32).reshape(seq_rows, heads_here, DK) * DK ** (-0.5)
    head_out = jnp.einsum("bhk,bhkv->bhv", query_heads, new_state, precision=lax.Precision.HIGHEST)
    gate_heads = out_gate.astype(F32).reshape(seq_rows, heads_here, DV)
    mixed = head_out * lax.rsqrt(jnp.mean(head_out * head_out, axis=-1, keepdims=True) + epsilon)
    mixed = (mixed * head_gain.astype(F32) * jax.nn.silu(gate_heads)).astype(BF16)
    mixed = mixed.reshape(seq_rows, heads_here * DV)
    updated_rows = tail(kv, tp, mixed, hidden_rows, mlp_gain, w_out, w_up, w_down)
    return (updated_rows, new_state.reshape(seq_rows, heads_here * DK * DV))


def solution(mesh):
    return jax.shard_map(
        functools.partial(body, mesh.shape["kv"], mesh.shape["tp"]),
        mesh=mesh,
        in_specs=(
            P("kv", "tp"),
            P("kv", "tp"),
            P(),
            P("kv", "tp"),
            P("kv", "tp"),
            P("kv", "tp"),
            P("kv", "tp"),
            P("kv", "tp"),
            P("tp"),
            P(),
            P("tp", "kv"),
            P("tp"),
            P("tp", "kv"),
            P("kv", "tp"),
        ),
        out_specs=(P("kv", "tp"), P("kv", "tp")),
        check_vma=False,
    )
```

```python
import functools

import jax
import jax.numpy as jnp
from jax import lax
from jax.experimental import pallas as pl
from jax.experimental.pallas import tpu as pltpu
from jax.sharding import PartitionSpec as P

DK = 128
DV = 256

epsilon = 1e-06
decay_normalizer = 16.0

F32 = jnp.float32
BF16 = jnp.bfloat16
MESH = pl.DeviceIdType.MESH


def remote(src, dst, send_sem, recv_sem, i, j):
    return pltpu.make_async_remote_copy(
        src_ref=src,
        dst_ref=dst,
        send_sem=send_sem,
        recv_sem=recv_sem,
        device_id={"kv": i, "tp": j},
        device_id_type=MESH,
    )


def dot(a, b):
    return jnp.dot(a, b, preferred_element_type=F32)


def inner_size(kv):
    size = 1
    while (size * 2) ** 2 <= kv:
        size = size * 2
    return size


def project_kernel(
    kv, tp, h_ref, g_ref, w0, w1, w2, w3, w4, o0, o1, o2, o3, o4,
    xbuf, v0, v1, v2, v3, v4, s0, s1, s2, s3, s4, r0, r1, r2, r3, r4,
    t0, t1, t2, t3, t4, u0, u1, u2, u3, u4,
    ssq, wsem, xs_sem, xr_sem, ss_sem, sr_sem, ps_sem, pr_sem, qs_sem, qr_sem,
):
    i, j = lax.axis_index("kv"), lax.axis_index("tp")
    ny = inner_size(kv)
    nz = kv // ny
    z, y = i // ny, lax.rem(i, ny)
    ratio = kv // tp
    rows = h_ref.shape[0]
    width = xbuf.shape[2]
    owner = i // ratio
    ws, vs, outs = (w0, w1, w2, w3, w4), (v0, v1, v2, v3, v4), (o0, o1, o2, o3, o4)
    sends, recvs = (s0, s1, s2, s3, s4), (r0, r1, r2, r3, r4)
    sums, finals = (t0, t1, t2, t3, t4), (u0, u1, u2, u3, u4)
    order = (3, 4, 1, 0, 2)
    loads = [pltpu.make_async_copy(w, v, wsem.at[n]) for n, (w, v) in enumerate(zip(ws, vs))]

    hidden_sends = []
    for a in range(ratio):
        for s in range(tp):
            dst_i, dst_j = j * ratio + a, lax.rem(j + s, tp)
            src = h_ref.at[:, pl.ds(a * width, width)]
            copy = remote(
                src, xbuf.at[i], xs_sem.at[a * tp + s], xr_sem.at[i], dst_i, dst_j
            )
            hidden_sends.append((a, s, dst_i, copy))
    for a, s, dst_i, copy in hidden_sends:
        if s:
            copy.start()
        else:
            pl.when(dst_i != i)(copy.start)
    for n in order:
        loads[n].start()

    hidden = h_ref[...].astype(F32)
    ssq[j] = jnp.broadcast_to(jnp.sum(hidden * hidden, axis=1, keepdims=True), (rows, 128))
    for a, s, dst_i, copy in hidden_sends:
        if not s:

            @pl.when(dst_i == i)
            def _():
                xbuf[i] = h_ref[:, a * width : (a + 1) * width]

    for s in range(kv):
        k = lax.rem(i + s, kv)
        arrive = remote(xbuf.at[k], xbuf.at[k], xs_sem.at[0], xr_sem.at[k], k, owner)
        if s:
            arrive.wait_recv()
        else:
            pl.when(owner != j)(arrive.wait_recv)

    square_sends = [
        remote(ssq.at[j], ssq.at[j], ss_sem.at[s], sr_sem.at[j], i, lax.rem(j + s, tp))
        for s in range(1, tp)
    ]
    gain = g_ref[:, pl.ds(pl.multiple_of(i * width, 128), width)].astype(F32)
    x = (xbuf[...].reshape(kv * rows, width).astype(F32) * gain).astype(BF16)
    part_sends = []
    for n in order:
        loads[n].wait()
        part = dot(x, vs[n][...]).astype(BF16)
        for zz in range(nz):
            for yy in range(ny):
                low = (zz * ny + yy) * rows
                sends[n][yy, zz] = part[low : low + rows]
        for s in range(1, ny):
            yy = lax.rem(y + s, ny)
            copy = remote(
                sends[n].at[yy], recvs[n].at[y], ps_sem.at[n, s], pr_sem.at[n, y], z * ny + yy, j
            )
            copy.start()
            part_sends.append(copy)
    for copy in square_sends:
        copy.start()
    for n in order:
        acc = sends[n][y].astype(F32)
        for s in range(1, ny):
            yy = lax.rem(y + s, ny)
            remote(
                recvs[n].at[yy], recvs[n].at[yy], ps_sem.at[n, 0], pr_sem.at[n, yy], z * ny + yy, j
            ).wait_recv()
            acc = acc + recvs[n][yy].astype(F32)
        sums[n][...] = acc.astype(BF16)
        for s in range(1, nz):
            zz = lax.rem(z + s, nz)
            copy = remote(
                sums[n].at[zz], finals[n].at[z], qs_sem.at[n, s], qr_sem.at[n, z], zz * ny + y, j
            )
            copy.start()
            part_sends.append(copy)
    for s in range(1, tp):
        k = lax.rem(j + s, tp)
        remote(ssq.at[k], ssq.at[k], ss_sem.at[0], sr_sem.at[k], i, k).wait_recv()
    total = ssq[0]
    for s in range(1, tp):
        total = total + ssq[s]
    scale = lax.rsqrt(total[:, :1] / (kv * width) + epsilon)
    for n in order:
        acc = sums[n][z].astype(F32)
        for s in range(1, nz):
            zz = lax.rem(z + s, nz)
            remote(
                finals[n].at[zz], finals[n].at[zz], qs_sem.at[n, 0], qr_sem.at[n, zz], zz * ny + y, j
            ).wait_recv()
            acc = acc + finals[n][zz].astype(F32)
        outs[n][...] = (acc * scale).astype(BF16)
    for a, s, dst_i, copy in hidden_sends:
        if s:
            copy.wait_send()
        else:
            pl.when(dst_i != i)(copy.wait_send)
    for copy in square_sends + part_sends:
        copy.wait_send()


def project(kv, tp, hidden_rows, norm_gain, weights):
    rows = hidden_rows.shape[0]
    width = weights[0].shape[0]
    ny = inner_size(kv)
    nz = kv // ny
    vmem = pl.BlockSpec(memory_space=pltpu.VMEM)
    anywhere = pl.BlockSpec(memory_space=pl.ANY)
    slots = [pltpu.VMEM((ny, nz, rows, w.shape[1]), BF16) for w in weights]
    lines = [pltpu.VMEM((nz, rows, w.shape[1]), BF16) for w in weights]
    dma = pltpu.SemaphoreType.DMA
    return pl.pallas_call(
        functools.partial(project_kernel, kv, tp),
        out_shape=[jax.ShapeDtypeStruct((rows, w.shape[1]), BF16) for w in weights],
        in_specs=[vmem] * 2 + [anywhere] * 5,
        out_specs=[vmem] * 5,
        scratch_shapes=[pltpu.VMEM((kv, rows, width), BF16)]
        + [pltpu.VMEM(w.shape, BF16) for w in weights]
        + slots
        + slots
        + lines
        + lines
        + [
            pltpu.VMEM((tp, rows, 128), F32),
            dma((5,)),
            dma((kv,)),
            dma((kv,)),
            dma((tp,)),
            dma((tp,)),
            dma((5, ny)),
            dma((5, ny)),
            dma((5, nz)),
            dma((5, nz)),
        ],
        compiler_params=pltpu.CompilerParams(
            has_side_effects=True, vmem_limit_bytes=62 * 1024 * 1024
        ),
        name="project",
    )(hidden_rows, norm_gain.reshape(1, -1), *weights)


PARTS = 2
CHUNKS = 2


def state_kernel(
    q_ref, k_ref, d_ref, v_ref, g_ref, bias_ref, gain_ref, old_ref, new_ref, mixed_ref,
    query, key, decay, total,
):
    part = pl.program_id(1)
    channels = DK // PARTS

    @pl.when(part == 0)
    def _():
        pre = d_ref[...].astype(F32) + bias_ref[...]
        log_decay = jnp.minimum(pre, 0.0) - jnp.log1p(jnp.exp(-jnp.abs(pre)))
        decay[...] = jnp.exp(log_decay / decay_normalizer)
        query[...] = q_ref[...].astype(F32) * DK ** (-0.5)
        key[...] = k_ref[...].astype(F32)
        total[...] = jnp.zeros_like(total)

    value = v_ref[...].astype(F32)
    acc = total[...]
    q, k, d = query[...], key[...], decay[...]
    for c in range(channels):
        at = slice(c * DV, (c + 1) * DV)
        new = d[:, c : c + 1] * old_ref[:, at] + k[:, c : c + 1] * value
        new_ref[:, at] = new
        acc = acc + q[:, c : c + 1] * new
    total[...] = acc
    query[...] = pltpu.roll(q, DK - channels, 1)
    key[...] = pltpu.roll(k, DK - channels, 1)
    decay[...] = pltpu.roll(d, DK - channels, 1)

    @pl.when(part == PARTS - 1)
    def _():
        gate = g_ref[...].astype(F32)
        mixed = acc * lax.rsqrt(jnp.mean(acc * acc, axis=1, keepdims=True) + epsilon)
        mixed_ref[...] = (mixed * gain_ref[...].astype(F32) * jax.nn.silu(gate)).astype(BF16)


def state(queries, keys_new, decay_pre, values, out_gate, decay_bias, head_gain, carried):
    rows, total = carried.shape
    heads = total // (DK * DV)
    narrow = pl.BlockSpec((rows, DK), lambda h, p: (0, h))
    wide = pl.BlockSpec((rows, DV), lambda h, p: (0, h))
    block = pl.BlockSpec((rows, DK * DV // PARTS), lambda h, p: (0, h * PARTS + p))
    return pl.pallas_call(
        state_kernel,
        grid=(heads, PARTS),
        out_shape=[
            jax.ShapeDtypeStruct(carried.shape, F32),
            jax.ShapeDtypeStruct((rows, heads * DV), BF16),
        ],
        in_specs=[narrow] * 3
        + [wide] * 2
        + [
            pl.BlockSpec((1, DK), lambda h, p: (0, h)),
            pl.BlockSpec((1, DV), lambda h, p: (0, 0)),
            block,
        ],
        out_specs=[block, wide],
        scratch_shapes=[pltpu.VMEM((rows, DK), F32)] * 3 + [pltpu.VMEM((rows, DV), F32)],
        compiler_params=pltpu.CompilerParams(vmem_limit_bytes=62 * 1024 * 1024),
        name="state",
    )(
        queries, keys_new, decay_pre, values, out_gate,
        decay_bias.reshape(1, -1), head_gain.reshape(1, -1), carried,
    )


def tail_kernel(
    kv, tp, mixed_ref, h_ref, g_ref, wo, wu, wd, out_ref,
    vo, vu, vd, mall, psend, precv, resid, rall, ssq, usend, urecv, xsend, xrecv, act, dsend, drecv,
    wsem, ms_sem, mr_sem, ps_sem, pr_sem, rs_sem, rr_sem, ss_sem, sr_sem,
    us_sem, ur_sem, xs_sem, xr_sem, as_sem, ar_sem, ds_sem, dr_sem,
):
    i, j = lax.axis_index("kv"), lax.axis_index("tp")
    ratio = kv // tp
    rows, columns = h_ref.shape
    width = columns // ratio
    owner = i // ratio
    loads = [
        pltpu.make_async_copy(w, v, wsem.at[n])
        for n, (w, v) in enumerate(((wo, vo), (wu, vu), (wd, vd)))
    ]
    sent = []

    def everyone(src_of, dst, send_sem, recv_sem):
        for s in range(1, kv):
            k = lax.rem(i + s, kv)
            copy = remote(src_of(k), dst.at[i], send_sem.at[s], recv_sem.at[i], k, j)
            copy.start()
            sent.append(copy)

    def arrived(dst, send_sem, recv_sem, s):
        k = lax.rem(i + s, kv)
        remote(dst.at[k], dst.at[k], send_sem.at[0], recv_sem.at[k], k, j).wait_recv()
        return k

    everyone(lambda k: mixed_ref, mall, ms_sem, mr_sem)
    for load in loads:
        load.start()
    mall[i] = mixed_ref[...]
    for s in range(1, kv):
        arrived(mall, ms_sem, mr_sem, s)
    loads[0].wait()
    part = dot(mall[...].reshape(kv * rows, mall.shape[2]), vo[...]).astype(BF16)
    psend[...] = part.reshape(psend.shape)

    slot = j * ratio + lax.rem(i, ratio)
    own_send = remote(psend.at[i], precv.at[slot], ps_sem.at[0], pr_sem.at[slot], i, owner)
    for s in range(1, kv):
        k = lax.rem(i + s, kv)
        copy = remote(psend.at[k], precv.at[slot], ps_sem.at[s], pr_sem.at[slot], k, owner)
        copy.start()
        sent.append(copy)
    pl.when(owner != j)(own_send.start)

    @pl.when(owner == j)
    def _():
        precv[slot] = psend[i]

    pieces = []
    for a in range(ratio):
        src_i = j * ratio + a
        attn = None
        for s in range(tp):
            src_j = lax.rem(j + s, tp)
            at = src_j * ratio + a
            arrive = remote(precv.at[at], precv.at[at], ps_sem.at[0], pr_sem.at[at], src_i, src_j)
            if s:
                arrive.wait_recv()
            else:
                pl.when(src_i != i)(arrive.wait_recv)
            term = precv[at].astype(F32)
            attn = term if attn is None else attn + term
        hidden = h_ref[:, a * width : (a + 1) * width].astype(F32)
        piece = (hidden + attn.astype(BF16).astype(F32)).astype(BF16)
        resid[:, a * width : (a + 1) * width] = piece
        piece = piece.astype(F32)
        pieces.append(jnp.sum(piece * piece, axis=1, keepdims=True))

    everyone(lambda k: resid, rall, rs_sem, rr_sem)
    ssq[j] = jnp.broadcast_to(sum(pieces), (rows, 128))
    rall[i] = resid[...]
    loads[1].wait()
    for s in range(1, kv):
        arrived(rall, rs_sem, rr_sem, s)
    for s in range(1, tp):
        copy = remote(ssq.at[j], ssq.at[j], ss_sem.at[s], sr_sem.at[j], i, lax.rem(j + s, tp))
        copy.start()
        sent.append(copy)
    x = (rall[...].reshape(kv * rows, columns).astype(F32) * g_ref[...].astype(F32)).astype(BF16)

    half = vu.shape[1] // 2
    piece = half // CHUNKS
    core, across = lax.rem(j, 2), j // 2
    other = 1 - core
    partner = across * 2 + other

    def columns_of(h, c):
        return pl.ds(pl.multiple_of(h * half + c * piece, 128), piece)

    for c in range(CHUNKS):
        usend[c] = dot(x, vu[:, columns_of(other, c)]).astype(BF16)
        copy = remote(usend.at[c], urecv.at[c], us_sem.at[c], ur_sem.at[c], i, partner)
        copy.start()
        sent.append(copy)
    for c in range(CHUNKS):
        mine = dot(x, vu[:, columns_of(core, c)])
        remote(urecv.at[c], urecv.at[c], us_sem.at[c], ur_sem.at[c], i, partner).wait_recv()
        xsend[c] = (mine + urecv[c].astype(F32)).astype(BF16)
        for s in range(1, tp // 2):
            to = lax.rem(across + s, tp // 2)
            copy = remote(
                xsend.at[c],
                xrecv.at[across, c],
                xs_sem.at[s, c],
                xr_sem.at[across, c],
                i,
                to * 2 + core,
            )
            copy.start()
            sent.append(copy)
    loads[2].wait()
    down = None
    for c in range(CHUNKS):
        total = xsend[c].astype(F32)
        for s in range(1, tp // 2):
            at = lax.rem(across + s, tp // 2)
            slot_ref = xrecv.at[at, c]
            remote(
                slot_ref, slot_ref, xs_sem.at[0, c], xr_sem.at[at, c], i, at * 2 + core
            ).wait_recv()
            total = total + xrecv[at, c].astype(F32)
        act[core, c] = jnp.square(jnp.maximum(total, 0.0)).astype(BF16)
        copy = remote(
            act.at[core, c], act.at[core, c], as_sem.at[c], ar_sem.at[core, c], i, partner
        )
        copy.start()
        sent.append(copy)
        term = dot(act[core, c], vd[columns_of(core, c), :])
        down = term if down is None else down + term
        arrive = act.at[other, c]
        remote(arrive, arrive, as_sem.at[c], ar_sem.at[other, c], i, partner).wait_recv()
        down = down + dot(act[other, c], vd[columns_of(other, c), :])
    dsend[...] = down.astype(BF16).reshape(dsend.shape)
    everyone(lambda k: dsend.at[k], drecv, ds_sem, dr_sem)

    for s in range(1, tp):
        k = lax.rem(j + s, tp)
        remote(ssq.at[k], ssq.at[k], ss_sem.at[0], sr_sem.at[k], i, k).wait_recv()
    squares = ssq[0]
    for s in range(1, tp):
        squares = squares + ssq[s]
    scale = lax.rsqrt(squares[:, :1] / (columns * tp) + epsilon)
    acc = dsend[i].astype(F32)
    for s in range(1, kv):
        k = arrived(drecv, ds_sem, dr_sem, s)
        acc = acc + drecv[k].astype(F32)
    acc = (acc * (scale * scale)).astype(BF16)
    out_ref[...] = (resid[...].astype(F32) + acc.astype(F32)).astype(BF16)
    pl.when(owner != j)(own_send.wait_send)
    for copy in sent:
        copy.wait_send()


def tail(kv, tp, mixed, hidden_rows, mlp_gain, w_out, w_up, w_down):
    rows, columns = hidden_rows.shape
    width = w_out.shape[1]
    ratio = kv // tp
    half = w_up.shape[1] // 2
    everything = kv * rows
    vmem = pl.BlockSpec(memory_space=pltpu.VMEM)
    anywhere = pl.BlockSpec(memory_space=pl.ANY)
    dma = pltpu.SemaphoreType.DMA
    return pl.pallas_call(
        functools.partial(tail_kernel, kv, tp),
        out_shape=jax.ShapeDtypeStruct((rows, columns), BF16),
        in_specs=[vmem] * 3 + [anywhere] * 3,
        out_specs=vmem,
        scratch_shapes=[
            pltpu.VMEM(w_out.shape, BF16),
            pltpu.VMEM(w_up.shape, BF16),
            pltpu.VMEM(w_down.shape, BF16),
            pltpu.VMEM((kv, rows, mixed.shape[1]), BF16),
            pltpu.VMEM((kv, rows, width), BF16),
            pltpu.VMEM((tp * ratio, rows, width), BF16),
            pltpu.VMEM((rows, columns), BF16),
            pltpu.VMEM((kv, rows, columns), BF16),
            pltpu.VMEM((tp, rows, 128), F32),
            pltpu.VMEM((CHUNKS, everything, half // CHUNKS), BF16),
            pltpu.VMEM((CHUNKS, everything, half // CHUNKS), BF16),
            pltpu.VMEM((CHUNKS, everything, half // CHUNKS), BF16),
            pltpu.VMEM((tp // 2, CHUNKS, everything, half // CHUNKS), BF16),
            pltpu.VMEM((2, CHUNKS, everything, half // CHUNKS), BF16),
            pltpu.VMEM((kv, rows, columns), BF16),
            pltpu.VMEM((kv, rows, columns), BF16),
            dma((3,)),
            dma((kv,)),
            dma((kv,)),
            dma((kv,)),
            dma((tp * ratio,)),
            dma((kv,)),
            dma((kv,)),
            dma((tp,)),
            dma((tp,)),
            dma((CHUNKS,)),
            dma((CHUNKS,)),
            dma((tp // 2, CHUNKS)),
            dma((tp // 2, CHUNKS)),
            dma((CHUNKS,)),
            dma((2, CHUNKS)),
            dma((kv,)),
            dma((kv,)),
        ],
        compiler_params=pltpu.CompilerParams(
            has_side_effects=True, vmem_limit_bytes=62 * 1024 * 1024
        ),
        name="tail",
    )(mixed, hidden_rows, mlp_gain.reshape(1, -1), w_out, w_up, w_down)


def body(
    kv,
    tp,
    hidden_rows,
    carried_state,
    norm_gain,
    w_query,
    w_key,
    w_decay,
    w_value,
    w_gate,
    decay_bias,
    head_gain,
    w_out,
    mlp_gain,
    w_up,
    w_down,
):
    queries, keys_new, decay_pre, values, out_gate = project(
        kv, tp, hidden_rows, norm_gain, (w_query, w_key, w_decay, w_value, w_gate)
    )
    new_state, mixed = state(
        queries, keys_new, decay_pre, values, out_gate, decay_bias, head_gain, carried_state
    )
    updated_rows = tail(kv, tp, mixed, hidden_rows, mlp_gain, w_out, w_up, w_down)
    return (updated_rows, new_state)


def solution(mesh):
    return jax.shard_map(
        functools.partial(body, mesh.shape["kv"], mesh.shape["tp"]),
        mesh=mesh,
        in_specs=(
            P("kv", "tp"),
            P("kv", "tp"),
            P(),
            P("kv", "tp"),
            P("kv", "tp"),
            P("kv", "tp"),
            P("kv", "tp"),
            P("kv", "tp"),
            P("tp"),
            P(),
            P("tp", "kv"),
            P("tp"),
            P("tp", "kv"),
            P("kv", "tp"),
        ),
        out_specs=(P("kv", "tp"), P("kv", "tp")),
        check_vma=False,
    )
```

```python
import functools

import jax
import jax.numpy as jnp
from jax import lax
from jax.experimental import pallas as pl
from jax.experimental.pallas import tpu as pltpu
from jax.sharding import PartitionSpec as P

DK = 128
DV = 256

epsilon = 1e-06
decay_normalizer = 16.0

F32 = jnp.float32
BF16 = jnp.bfloat16
MESH = pl.DeviceIdType.MESH


def remote(src, dst, send_sem, recv_sem, i, j):
    return pltpu.make_async_remote_copy(
        src_ref=src,
        dst_ref=dst,
        send_sem=send_sem,
        recv_sem=recv_sem,
        device_id={"kv": i, "tp": j},
        device_id_type=MESH,
    )


def dot(a, b):
    return jnp.dot(a, b, preferred_element_type=F32)


def inner_size(kv):
    size = 1
    while (size * 2) ** 2 <= kv:
        size = size * 2
    return size


def project_kernel(
    kv, tp, h_ref, g_ref, w0, w1, w2, w3, w4, o0, o1, o2, o3, o4,
    xbuf, v0, v1, v2, v3, v4, s0, s1, s2, s3, s4, r0, r1, r2, r3, r4,
    t0, t1, t2, t3, t4, u0, u1, u2, u3, u4,
    ssq, wsem, xs_sem, xr_sem, ss_sem, sr_sem, ps_sem, pr_sem, qs_sem, qr_sem,
):
    i, j = lax.axis_index("kv"), lax.axis_index("tp")
    ny = inner_size(kv)
    nz = kv // ny
    z, y = i // ny, lax.rem(i, ny)
    ratio = kv // tp
    rows = h_ref.shape[0]
    width = xbuf.shape[2]
    owner = i // ratio
    ws, vs, outs = (w0, w1, w2, w3, w4), (v0, v1, v2, v3, v4), (o0, o1, o2, o3, o4)
    sends, recvs = (s0, s1, s2, s3, s4), (r0, r1, r2, r3, r4)
    sums, finals = (t0, t1, t2, t3, t4), (u0, u1, u2, u3, u4)
    order = (3, 4, 1, 0, 2)
    loads = [pltpu.make_async_copy(w, v, wsem.at[n]) for n, (w, v) in enumerate(zip(ws, vs))]

    hidden_sends = []
    for a in range(ratio):
        for s in range(tp):
            dst_i, dst_j = j * ratio + a, lax.rem(j + s, tp)
            src = h_ref.at[:, pl.ds(a * width, width)]
            copy = remote(
                src, xbuf.at[i], xs_sem.at[a * tp + s], xr_sem.at[i], dst_i, dst_j
            )
            hidden_sends.append((a, s, dst_i, copy))
    for a, s, dst_i, copy in hidden_sends:
        if s:
            copy.start()
        else:
            pl.when(dst_i != i)(copy.start)
    for n in order:
        loads[n].start()

    hidden = h_ref[...].astype(F32)
    ssq[j] = jnp.broadcast_to(jnp.sum(hidden * hidden, axis=1, keepdims=True), (rows, 128))
    for a, s, dst_i, copy in hidden_sends:
        if not s:

            @pl.when(dst_i == i)
            def _():
                xbuf[i] = h_ref[:, a * width : (a + 1) * width]

    for s in range(kv):
        k = lax.rem(i + s, kv)
        arrive = remote(xbuf.at[k], xbuf.at[k], xs_sem.at[0], xr_sem.at[k], k, owner)
        if s:
            arrive.wait_recv()
        else:
            pl.when(owner != j)(arrive.wait_recv)

    square_sends = [
        remote(ssq.at[j], ssq.at[j], ss_sem.at[s], sr_sem.at[j], i, lax.rem(j + s, tp))
        for s in range(1, tp)
    ]
    gain = g_ref[:, pl.ds(pl.multiple_of(i * width, 128), width)].astype(F32)
    x = (xbuf[...].reshape(kv * rows, width).astype(F32) * gain).astype(BF16)
    part_sends = []
    for n in order:
        loads[n].wait()
        part = dot(x, vs[n][...]).astype(BF16)
        for zz in range(nz):
            for yy in range(ny):
                low = (zz * ny + yy) * rows
                sends[n][yy, zz] = part[low : low + rows]
        for s in range(1, ny):
            yy = lax.rem(y + s, ny)
            copy = remote(
                sends[n].at[yy], recvs[n].at[y], ps_sem.at[n, s], pr_sem.at[n, y], z * ny + yy, j
            )
            copy.start()
            part_sends.append(copy)
    for copy in square_sends:
        copy.start()
    for n in order:
        acc = sends[n][y].astype(F32)
        for s in range(1, ny):
            yy = lax.rem(y + s, ny)
            remote(
                recvs[n].at[yy], recvs[n].at[yy], ps_sem.at[n, 0], pr_sem.at[n, yy], z * ny + yy, j
            ).wait_recv()
            acc = acc + recvs[n][yy].astype(F32)
        sums[n][...] = acc.astype(BF16)
        for s in range(1, nz):
            zz = lax.rem(z + s, nz)
            copy = remote(
                sums[n].at[zz], finals[n].at[z], qs_sem.at[n, s], qr_sem.at[n, z], zz * ny + y, j
            )
            copy.start()
            part_sends.append(copy)
    for s in range(1, tp):
        k = lax.rem(j + s, tp)
        remote(ssq.at[k], ssq.at[k], ss_sem.at[0], sr_sem.at[k], i, k).wait_recv()
    total = ssq[0]
    for s in range(1, tp):
        total = total + ssq[s]
    scale = lax.rsqrt(total[:, :1] / (kv * width) + epsilon)
    for n in order:
        acc = sums[n][z].astype(F32)
        for s in range(1, nz):
            zz = lax.rem(z + s, nz)
            remote(
                finals[n].at[zz], finals[n].at[zz], qs_sem.at[n, 0], qr_sem.at[n, zz], zz * ny + y, j
            ).wait_recv()
            acc = acc + finals[n][zz].astype(F32)
        outs[n][...] = (acc * scale).astype(BF16)
    for a, s, dst_i, copy in hidden_sends:
        if s:
            copy.wait_send()
        else:
            pl.when(dst_i != i)(copy.wait_send)
    for copy in square_sends + part_sends:
        copy.wait_send()


def project(kv, tp, hidden_rows, norm_gain, weights):
    rows = hidden_rows.shape[0]
    width = weights[0].shape[0]
    ny = inner_size(kv)
    nz = kv // ny
    vmem = pl.BlockSpec(memory_space=pltpu.VMEM)
    anywhere = pl.BlockSpec(memory_space=pl.ANY)
    slots = [pltpu.VMEM((ny, nz, rows, w.shape[1]), BF16) for w in weights]
    lines = [pltpu.VMEM((nz, rows, w.shape[1]), BF16) for w in weights]
    dma = pltpu.SemaphoreType.DMA
    return pl.pallas_call(
        functools.partial(project_kernel, kv, tp),
        out_shape=[jax.ShapeDtypeStruct((rows, w.shape[1]), BF16) for w in weights],
        in_specs=[vmem] * 2 + [anywhere] * 5,
        out_specs=[vmem] * 5,
        scratch_shapes=[pltpu.VMEM((kv, rows, width), BF16)]
        + [pltpu.VMEM(w.shape, BF16) for w in weights]
        + slots
        + slots
        + lines
        + lines
        + [
            pltpu.VMEM((tp, rows, 128), F32),
            dma((5,)),
            dma((kv,)),
            dma((kv,)),
            dma((tp,)),
            dma((tp,)),
            dma((5, ny)),
            dma((5, ny)),
            dma((5, nz)),
            dma((5, nz)),
        ],
        compiler_params=pltpu.CompilerParams(
            has_side_effects=True, vmem_limit_bytes=62 * 1024 * 1024
        ),
        name="project",
    )(hidden_rows, norm_gain.reshape(1, -1), *weights)


PARTS = 2
CHUNKS = 4


def state_kernel(
    q_ref, k_ref, d_ref, v_ref, g_ref, bias_ref, gain_ref, old_ref, new_ref, mixed_ref,
    query, key, decay, total,
):
    part = pl.program_id(1)
    channels = DK // PARTS

    @pl.when(part == 0)
    def _():
        pre = d_ref[...].astype(F32) + bias_ref[...]
        log_decay = jnp.minimum(pre, 0.0) - jnp.log1p(jnp.exp(-jnp.abs(pre)))
        decay[...] = jnp.exp(log_decay / decay_normalizer)
        query[...] = q_ref[...].astype(F32) * DK ** (-0.5)
        key[...] = k_ref[...].astype(F32)
        total[...] = jnp.zeros_like(total)

    value = v_ref[...].astype(F32)
    acc = total[...]
    q, k, d = query[...], key[...], decay[...]
    for c in range(channels):
        at = slice(c * DV, (c + 1) * DV)
        new = d[:, c : c + 1] * old_ref[:, at] + k[:, c : c + 1] * value
        new_ref[:, at] = new
        acc = acc + q[:, c : c + 1] * new
    total[...] = acc
    query[...] = pltpu.roll(q, DK - channels, 1)
    key[...] = pltpu.roll(k, DK - channels, 1)
    decay[...] = pltpu.roll(d, DK - channels, 1)

    @pl.when(part == PARTS - 1)
    def _():
        gate = g_ref[...].astype(F32)
        mixed = acc * lax.rsqrt(jnp.mean(acc * acc, axis=1, keepdims=True) + epsilon)
        mixed_ref[...] = (mixed * gain_ref[...].astype(F32) * jax.nn.silu(gate)).astype(BF16)


def state(queries, keys_new, decay_pre, values, out_gate, decay_bias, head_gain, carried):
    rows, total = carried.shape
    heads = total // (DK * DV)
    narrow = pl.BlockSpec((rows, DK), lambda h, p: (0, h))
    wide = pl.BlockSpec((rows, DV), lambda h, p: (0, h))
    block = pl.BlockSpec((rows, DK * DV // PARTS), lambda h, p: (0, h * PARTS + p))
    return pl.pallas_call(
        state_kernel,
        grid=(heads, PARTS),
        out_shape=[
            jax.ShapeDtypeStruct(carried.shape, F32),
            jax.ShapeDtypeStruct((rows, heads * DV), BF16),
        ],
        in_specs=[narrow] * 3
        + [wide] * 2
        + [
            pl.BlockSpec((1, DK), lambda h, p: (0, h)),
            pl.BlockSpec((1, DV), lambda h, p: (0, 0)),
            block,
        ],
        out_specs=[block, wide],
        scratch_shapes=[pltpu.VMEM((rows, DK), F32)] * 3 + [pltpu.VMEM((rows, DV), F32)],
        compiler_params=pltpu.CompilerParams(vmem_limit_bytes=62 * 1024 * 1024),
        name="state",
    )(
        queries, keys_new, decay_pre, values, out_gate,
        decay_bias.reshape(1, -1), head_gain.reshape(1, -1), carried,
    )


def tail_kernel(
    kv, tp, mixed_ref, h_ref, g_ref, wo, wu, wd, out_ref,
    vo, vu, vd, mall, psend, precv, resid, rall, ssq, usend, urecv, xsend, xrecv, act, dsend, drecv,
    wsem, ms_sem, mr_sem, ps_sem, pr_sem, rs_sem, rr_sem, ss_sem, sr_sem,
    us_sem, ur_sem, xs_sem, xr_sem, as_sem, ar_sem, ds_sem, dr_sem,
):
    i, j = lax.axis_index("kv"), lax.axis_index("tp")
    ratio = kv // tp
    rows, columns = h_ref.shape
    width = columns // ratio
    owner = i // ratio
    loads = [
        pltpu.make_async_copy(w, v, wsem.at[n])
        for n, (w, v) in enumerate(((wo, vo), (wu, vu), (wd, vd)))
    ]
    sent = []

    def everyone(src_of, dst, send_sem, recv_sem):
        for s in range(1, kv):
            k = lax.rem(i + s, kv)
            copy = remote(src_of(k), dst.at[i], send_sem.at[s], recv_sem.at[i], k, j)
            copy.start()
            sent.append(copy)

    def arrived(dst, send_sem, recv_sem, s):
        k = lax.rem(i + s, kv)
        remote(dst.at[k], dst.at[k], send_sem.at[0], recv_sem.at[k], k, j).wait_recv()
        return k

    everyone(lambda k: mixed_ref, mall, ms_sem, mr_sem)
    for load in loads:
        load.start()
    mall[i] = mixed_ref[...]
    for s in range(1, kv):
        arrived(mall, ms_sem, mr_sem, s)
    loads[0].wait()
    part = dot(mall[...].reshape(kv * rows, mall.shape[2]), vo[...]).astype(BF16)
    psend[...] = part.reshape(psend.shape)

    slot = j * ratio + lax.rem(i, ratio)
    own_send = remote(psend.at[i], precv.at[slot], ps_sem.at[0], pr_sem.at[slot], i, owner)
    for s in range(1, kv):
        k = lax.rem(i + s, kv)
        copy = remote(psend.at[k], precv.at[slot], ps_sem.at[s], pr_sem.at[slot], k, owner)
        copy.start()
        sent.append(copy)
    pl.when(owner != j)(own_send.start)

    @pl.when(owner == j)
    def _():
        precv[slot] = psend[i]

    pieces = []
    for a in range(ratio):
        src_i = j * ratio + a
        attn = None
        for s in range(tp):
            src_j = lax.rem(j + s, tp)
            at = src_j * ratio + a
            arrive = remote(precv.at[at], precv.at[at], ps_sem.at[0], pr_sem.at[at], src_i, src_j)
            if s:
                arrive.wait_recv()
            else:
                pl.when(src_i != i)(arrive.wait_recv)
            term = precv[at].astype(F32)
            attn = term if attn is None else attn + term
        hidden = h_ref[:, a * width : (a + 1) * width].astype(F32)
        piece = (hidden + attn.astype(BF16).astype(F32)).astype(BF16)
        resid[:, a * width : (a + 1) * width] = piece
        piece = piece.astype(F32)
        pieces.append(jnp.sum(piece * piece, axis=1, keepdims=True))

    everyone(lambda k: resid, rall, rs_sem, rr_sem)
    ssq[j] = jnp.broadcast_to(sum(pieces), (rows, 128))
    rall[i] = resid[...]
    loads[1].wait()
    for s in range(1, kv):
        arrived(rall, rs_sem, rr_sem, s)
    for s in range(1, tp):
        copy = remote(ssq.at[j], ssq.at[j], ss_sem.at[s], sr_sem.at[j], i, lax.rem(j + s, tp))
        copy.start()
        sent.append(copy)
    x = (rall[...].reshape(kv * rows, columns).astype(F32) * g_ref[...].astype(F32)).astype(BF16)

    half = vu.shape[1] // 2
    chunks = usend.shape[0]
    piece = half // chunks
    core, across = lax.rem(j, 2), j // 2
    other = 1 - core
    partner = across * 2 + other

    def columns_of(h, c):
        return pl.ds(pl.multiple_of(h * half + c * piece, 128), piece)

    def give(c):
        usend[c] = dot(x, vu[:, columns_of(other, c)]).astype(BF16)
        copy = remote(usend.at[c], urecv.at[c], us_sem.at[c], ur_sem.at[c], i, partner)
        copy.start()
        sent.append(copy)

    give(0)
    for c in range(chunks):
        if c + 1 < chunks:
            give(c + 1)
        mine = dot(x, vu[:, columns_of(core, c)])
        remote(urecv.at[c], urecv.at[c], us_sem.at[c], ur_sem.at[c], i, partner).wait_recv()
        xsend[c] = (mine + urecv[c].astype(F32)).astype(BF16)
        for s in range(1, tp // 2):
            to = lax.rem(across + s, tp // 2)
            copy = remote(
                xsend.at[c],
                xrecv.at[across, c],
                xs_sem.at[s, c],
                xr_sem.at[across, c],
                i,
                to * 2 + core,
            )
            copy.start()
            sent.append(copy)
    loads[2].wait()
    down = None
    for c in range(chunks):
        total = xsend[c].astype(F32)
        for s in range(1, tp // 2):
            at = lax.rem(across + s, tp // 2)
            slot_ref = xrecv.at[at, c]
            remote(
                slot_ref, slot_ref, xs_sem.at[0, c], xr_sem.at[at, c], i, at * 2 + core
            ).wait_recv()
            total = total + xrecv[at, c].astype(F32)
        act[core, c] = jnp.square(jnp.maximum(total, 0.0)).astype(BF16)
        copy = remote(
            act.at[core, c], act.at[core, c], as_sem.at[c], ar_sem.at[core, c], i, partner
        )
        copy.start()
        sent.append(copy)
        term = dot(act[core, c], vd[columns_of(core, c), :])
        down = term if down is None else down + term
        arrive = act.at[other, c]
        remote(arrive, arrive, as_sem.at[c], ar_sem.at[other, c], i, partner).wait_recv()
        down = down + dot(act[other, c], vd[columns_of(other, c), :])
    dsend[...] = down.astype(BF16).reshape(dsend.shape)
    everyone(lambda k: dsend.at[k], drecv, ds_sem, dr_sem)

    for s in range(1, tp):
        k = lax.rem(j + s, tp)
        remote(ssq.at[k], ssq.at[k], ss_sem.at[0], sr_sem.at[k], i, k).wait_recv()
    squares = ssq[0]
    for s in range(1, tp):
        squares = squares + ssq[s]
    scale = lax.rsqrt(squares[:, :1] / (columns * tp) + epsilon)
    acc = dsend[i].astype(F32)
    for s in range(1, kv):
        k = arrived(drecv, ds_sem, dr_sem, s)
        acc = acc + drecv[k].astype(F32)
    acc = (acc * (scale * scale)).astype(BF16)
    out_ref[...] = (resid[...].astype(F32) + acc.astype(F32)).astype(BF16)
    pl.when(owner != j)(own_send.wait_send)
    for copy in sent:
        copy.wait_send()


def tail(kv, tp, mixed, hidden_rows, mlp_gain, w_out, w_up, w_down):
    rows, columns = hidden_rows.shape
    width = w_out.shape[1]
    ratio = kv // tp
    half = w_up.shape[1] // 2
    everything = kv * rows
    chunks = max(1, min(CHUNKS, half // 128))
    vmem = pl.BlockSpec(memory_space=pltpu.VMEM)
    anywhere = pl.BlockSpec(memory_space=pl.ANY)
    dma = pltpu.SemaphoreType.DMA
    return pl.pallas_call(
        functools.partial(tail_kernel, kv, tp),
        out_shape=jax.ShapeDtypeStruct((rows, columns), BF16),
        in_specs=[vmem] * 3 + [anywhere] * 3,
        out_specs=vmem,
        scratch_shapes=[
            pltpu.VMEM(w_out.shape, BF16),
            pltpu.VMEM(w_up.shape, BF16),
            pltpu.VMEM(w_down.shape, BF16),
            pltpu.VMEM((kv, rows, mixed.shape[1]), BF16),
            pltpu.VMEM((kv, rows, width), BF16),
            pltpu.VMEM((tp * ratio, rows, width), BF16),
            pltpu.VMEM((rows, columns), BF16),
            pltpu.VMEM((kv, rows, columns), BF16),
            pltpu.VMEM((tp, rows, 128), F32),
            pltpu.VMEM((chunks, everything, half // chunks), BF16),
            pltpu.VMEM((chunks, everything, half // chunks), BF16),
            pltpu.VMEM((chunks, everything, half // chunks), BF16),
            pltpu.VMEM((tp // 2, chunks, everything, half // chunks), BF16),
            pltpu.VMEM((2, chunks, everything, half // chunks), BF16),
            pltpu.VMEM((kv, rows, columns), BF16),
            pltpu.VMEM((kv, rows, columns), BF16),
            dma((3,)),
            dma((kv,)),
            dma((kv,)),
            dma((kv,)),
            dma((tp * ratio,)),
            dma((kv,)),
            dma((kv,)),
            dma((tp,)),
            dma((tp,)),
            dma((chunks,)),
            dma((chunks,)),
            dma((tp // 2, chunks)),
            dma((tp // 2, chunks)),
            dma((chunks,)),
            dma((2, chunks)),
            dma((kv,)),
            dma((kv,)),
        ],
        compiler_params=pltpu.CompilerParams(
            has_side_effects=True, vmem_limit_bytes=62 * 1024 * 1024
        ),
        name="tail",
    )(mixed, hidden_rows, mlp_gain.reshape(1, -1), w_out, w_up, w_down)


def body(
    kv,
    tp,
    hidden_rows,
    carried_state,
    norm_gain,
    w_query,
    w_key,
    w_decay,
    w_value,
    w_gate,
    decay_bias,
    head_gain,
    w_out,
    mlp_gain,
    w_up,
    w_down,
):
    queries, keys_new, decay_pre, values, out_gate = project(
        kv, tp, hidden_rows, norm_gain, (w_query, w_key, w_decay, w_value, w_gate)
    )
    new_state, mixed = state(
        queries, keys_new, decay_pre, values, out_gate, decay_bias, head_gain, carried_state
    )
    updated_rows = tail(kv, tp, mixed, hidden_rows, mlp_gain, w_out, w_up, w_down)
    return (updated_rows, new_state)


def solution(mesh):
    return jax.shard_map(
        functools.partial(body, mesh.shape["kv"], mesh.shape["tp"]),
        mesh=mesh,
        in_specs=(
            P("kv", "tp"),
            P("kv", "tp"),
            P(),
            P("kv", "tp"),
            P("kv", "tp"),
            P("kv", "tp"),
            P("kv", "tp"),
            P("kv", "tp"),
            P("tp"),
            P(),
            P("tp", "kv"),
            P("tp"),
            P("tp", "kv"),
            P("kv", "tp"),
        ),
        out_specs=(P("kv", "tp"), P("kv", "tp")),
        check_vma=False,
    )
```
